32 devices in a mesh: sp: 16 (over z, y, x), tp: 2 (over core).
Axes of the slice: x: 2, y: 2, z: 4, core: 2. Of those that a mesh axis runs over, the one named last changes fastest.
Arguments:
- features: bfloat16 [8192, 4096], P('sp', 'tp'), may hold values from -6 to 6
- weight_value: bfloat16 [4096, 1024], P(None, 'tp'), may hold values from -0.09375 to 0.09375
- weight_gate: bfloat16 [4096, 1024], P(None, 'tp'), may hold values from -0.09375 to 0.09375
- weight_out: bfloat16 [4096, 1024], P(None, 'tp'), may hold values from -0.1875 to 0.1875
- conv_taps: float32 [31, 1024], P(None, 'tp'), may hold values from -6 to 6
- norm_gain: float32 [1024], P('tp'), may hold values from 0.1 to 1.9
- out_grad: bfloat16 [8192, 4096], P('sp', 'tp'), may hold values from -6 to 6
Outputs:
- value_grad: float32 [8192, 1024], P('sp', 'tp')
- gate_grad: float32 [8192, 1024], P('sp', 'tp')
- value_wgrad: float32 [4096, 1024], P('sp', 'tp')
- gate_wgrad: float32 [4096, 1024], P('sp', 'tp')
- out_wgrad: float32 [4096, 1024], P('sp', 'tp')
- taps_grad: float32 [31, 1024], P(None, 'tp')
- gain_grad: float32 [1024], P('tp')
The draws below stay inside these ranges and needn't reach their ends.
All inputs are finite; a program needn't handle non-finite values.
Results may differ from the reference program's by a relative error of at most 0.0057.
Values may be sent and summed in bfloat16 or wider, within the bound.
No kernel may reach another device: no remote copies, remote signals or barrier semaphores. Data moves between devices by JAX's collectives and lax.ppermute only.
A program may use at most 192 MiB of HBM per device.

```python
import math
import jax
import jax.numpy as jnp
from jax import lax

D = 4096
CH = 1024
KW = 31
TOKENS = 8192


def draw_conv_taps(key, part):
    base_key = jax.random.fold_in(key, 11)
    first_key, second_key, third_key = jax.random.split(base_key, 3)
    base = jnp.clip(jax.random.normal(first_key, (KW, CH), jnp.float32), -3.5, 3.5)
    spread = jnp.exp(jax.random.uniform(second_key, (CH,), jnp.float32, -0.7, 0.7))
    upper_big = jax.random.bernoulli(third_key)
    lower_half = jnp.arange(CH) < CH // 2
    block_scale = jnp.where(lower_half == upper_big, 3.5, 1.0)
    return base * spread * block_scale / math.sqrt(KW)


def strengthened(entries, own_key, source, target, shards_of, factor):
    owner, partner = [(jnp.arange(entries.shape[position]) // (entries.shape[position] // shards_of)).reshape([-1 if axis == position else 1 for axis in range(entries.ndim)]) for position in (source, target)]
    chosen = jax.random.permutation(own_key, shards_of)[partner]
    strong = (owner == chosen) | (owner == (partner + shards_of // 2) % shards_of)
    return jnp.where(strong, factor * entries, entries)


def shard_levels(key, shape, cuts, low, high):
    loudness = 1.0
    for position, blocks in cuts:
        heights = jax.random.uniform(jax.random.fold_in(jax.random.fold_in(key, 6), position), (blocks,), jnp.float32, low / len(cuts), high / len(cuts))
        loudness = loudness * jnp.repeat(jnp.exp(heights), shape[position] // blocks).reshape((-1,) + (1,) * (len(shape) - 1 - position))
    return loudness


def bell_draw(own_key, shape, deviation, most, cuts=(), held_as=jnp.bfloat16):
    result = deviation * jax.random.normal(own_key, shape, jnp.float32)
    if cuts:
        result = result * shard_levels(own_key, shape, cuts, -0.22, 0.18)
    return jnp.clip(result, -most, most).astype(held_as)


def noise_with(key, shape, scale, bound, shards, heavy, dtype=jnp.bfloat16):
    array = scale * jax.random.normal(key, shape, jnp.float32)
    if shards:
        array = array * shard_levels(key, shape, shards, -0.22, 0.18)
    return jnp.clip(strengthened(array, jax.random.fold_in(key, 3), *heavy), -bound, bound).astype(dtype)


def setup_inputs(seed: int = 0) -> dict:
    keys = jax.random.split(jax.random.key(seed), 8)
    return {
        "features": noise_with(keys[0], (TOKENS, D), 1.0, 6.0, ((0, 16), (1, 2)), (0, 1, 16, 2.0)),
        "weight_value": bell_draw(keys[1], (D, CH), D ** -0.5, 0.09375, ((1, 2),)),
        "weight_gate": bell_draw(keys[2], (D, CH), D ** -0.5, 0.09375, ((1, 2),)),
        "weight_out": bell_draw(keys[3], (D, CH), CH ** -0.5, 0.1875, ((1, 2),)),
        "conv_taps": draw_conv_taps(jax.random.fold_in(keys[7], 71), 0),
        "norm_gain": jnp.clip(1.0 + 0.18 * jax.random.normal(keys[5], (CH,), jnp.float32), 0.1, 1.9),
        "out_grad": noise_with(keys[6], (TOKENS, D), 1.0, 6.0, ((0, 16), (1, 2)), (0, 1, 16, 2.0)),
    }


NORM_EPS = 1e-05

def over_tokens(left_rows, right_rows):
    return lax.dot_general(left_rows, right_rows, (((0,), (0,)), ((), ())), preferred_element_type=jnp.float32)

def reference(features, weight_value, weight_gate, weight_out, conv_taps, norm_gain, out_grad):
    half_width = KW // 2
    seq_total = features.shape[0]
    value_half = jnp.dot(features, weight_value, preferred_element_type=jnp.float32).astype(jnp.bfloat16)
    gate_half = jnp.dot(features, weight_gate, preferred_element_type=jnp.float32).astype(jnp.bfloat16)
    value_half, gate_half = lax.optimization_barrier((value_half, gate_half))
    value_pre = value_half.astype(jnp.float32)
    gate_pre = gate_half.astype(jnp.float32)
    gate_sig = jax.nn.sigmoid(gate_pre)
    mixed_half = lax.optimization_barrier((value_pre * gate_sig).astype(jnp.bfloat16))
    padded = jnp.pad(mixed_half.astype(jnp.float32), ((half_width, half_width), (0, 0)))
    conv_out = jnp.zeros((seq_total, CH), jnp.float32)
    for offset in range(KW):
        conv_out = conv_out + conv_taps[offset] * padded[offset:offset + seq_total]
    mean_row = lax.optimization_barrier(jnp.sum(conv_out, axis=-1, keepdims=True)) / CH
    var_row = lax.optimization_barrier(jnp.sum(conv_out * conv_out, axis=-1, keepdims=True)) / CH - mean_row * mean_row
    inv_std = lax.rsqrt(var_row + NORM_EPS)
    normed = (conv_out - mean_row) * inv_std
    pre_act = normed * norm_gain
    act_sig = jax.nn.sigmoid(pre_act)
    act_half = (pre_act * act_sig).astype(jnp.bfloat16)
    act_grad = jnp.dot(out_grad, weight_out, preferred_element_type=jnp.float32)
    out_wgrad = over_tokens(out_grad, act_half)
    pre_grad = act_grad * act_sig * (1.0 + pre_act * (1.0 - act_sig))
    gain_grad = lax.optimization_barrier(jnp.sum(pre_grad * normed, axis=0))
    norm_grad = pre_grad * norm_gain
    first_mom = lax.optimization_barrier(jnp.sum(norm_grad, axis=-1, keepdims=True)) / CH
    second_mom = lax.optimization_barrier(jnp.sum(norm_grad * normed, axis=-1, keepdims=True)) / CH
    conv_grad = inv_std * (norm_grad - first_mom - normed * second_mom)
    grad_ext = jnp.pad(conv_grad, ((half_width, half_width), (0, 0)))
    mixed_grad = jnp.zeros((seq_total, CH), jnp.float32)
    taps_rows = []
    for offset in range(KW):
        begin = 2 * half_width - offset
        mixed_grad = mixed_grad + conv_taps[offset] * grad_ext[begin:begin + seq_total]
        taps_rows.append(lax.optimization_barrier(jnp.sum(conv_grad * padded[offset:offset + seq_total], axis=0)))
    taps_grad = jnp.stack(taps_rows)
    value_grad = mixed_grad * gate_sig
    gate_grad = mixed_grad * value_pre * gate_sig * (1.0 - gate_sig)
    value_wgrad = over_tokens(features, value_grad.astype(jnp.bfloat16))
    gate_wgrad = over_tokens(features, gate_grad.astype(jnp.bfloat16))
    return (value_grad, gate_grad, value_wgrad, gate_wgrad, out_wgrad, taps_grad, gain_grad)
```

```python
import functools

import jax
import jax.numpy as jnp
from jax import lax
from jax.experimental import pallas as pl
from jax.experimental.pallas import tpu as pltpu
from jax.sharding import PartitionSpec as P

NORM_EPS = 1e-05


def weight_kernel(ids_ref, mine_ref, other_ref, right_ref, *outs, edges):
    rows = outs[0].shape[2]
    blocks = outs[0].shape[0]
    half = mine_ref.shape[1] // rows

    def fill(left_ref, spot, out_ref, step, begin, end):
        columns = pl.ds(pl.multiple_of(spot * rows, rows), rows)
        term = jnp.dot(
            right_ref[begin:end], left_ref[:, columns], preferred_element_type=jnp.float32
        )
        out_ref[step] = term.astype(jnp.bfloat16)

    @pl.loop(0, blocks)
    def _(step):
        for k, out_ref in enumerate(outs):
            spot = ids_ref[k, step]
            near = spot < half
            begin, end = edges[k], edges[k + 1]

            @pl.when(near)
            def _():
                fill(mine_ref, spot, out_ref, step, begin, end)

            @pl.when(jnp.logical_not(near))
            def _():
                fill(other_ref, spot - half, out_ref, step, begin, end)


def weight_blocks(ids, mine, other, right, rows, edges):
    tokens = right.shape[1]
    blocks = ids.shape[1]
    if rows % 128:
        whole = jnp.concatenate([mine, other], axis=1).reshape(tokens, -1, rows)
        return [
            jnp.einsum(
                "ct,tbr->bcr", right[a:b], whole[:, spots], preferred_element_type=jnp.float32
            ).astype(jnp.bfloat16)
            for a, b, spots in zip(edges[:-1], edges[1:], ids)
        ]
    whole = pl.BlockSpec(memory_space=pltpu.VMEM)
    return pl.pallas_call(
        functools.partial(weight_kernel, edges=edges),
        in_specs=[pl.BlockSpec(memory_space=pltpu.SMEM), whole, whole, whole],
        out_specs=[whole] * ids.shape[0],
        out_shape=[
            jax.ShapeDtypeStruct((blocks, b - a, rows), jnp.bfloat16)
            for a, b in zip(edges[:-1], edges[1:])
        ],
        cost_estimate=pl.CostEstimate(
            flops=2 * tokens * rows * edges[-1] * blocks,
            bytes_accessed=4 * mine.size + 2 * right.size + 2 * blocks * edges[-1] * rows,
            transcendentals=0,
        ),
    )(ids, mine, other, right)


def add(terms):
    total = terms[0].astype(jnp.float32)
    for term in terms[1:]:
        total = total + term.astype(jnp.float32)
    return total


def flips_of(order):
    bits = len(order)
    return [
        sum(1 << bit for k, bit in enumerate(order) if not (p >> (bits - 1 - k)) & 1)
        for p in range(1 << bits)
    ]


def exchange_sum(sent, kept, order):
    count = 1 << len(order)
    kept = [kept]
    for step, bit in enumerate(order):
        got = lax.ppermute(sent, "sp", [(i, i ^ (1 << bit)) for i in range(count)])
        kept.append(got)
        size = got.shape[0]
        if step + 1 < len(order):
            sent = add([k[: size // 2] for k in kept]).astype(jnp.bfloat16)
            kept = [k[size // 2 :] for k in kept]
    return add([k[0] for k in kept])


def orders_of(count):
    bits = count.bit_length() - 1
    top = list(range(max(bits - 2, 0), bits))
    low = list(range(max(bits - 2, 0)))
    return top + low, low + top, low[::-1] + top


def scatter_rows(mine, other, right, splits, side, place, count):
    rows = 2 * mine.shape[1] // count
    columns = right.shape[0]
    edges = (0, *(columns * s // 16 for s in splits), columns)
    orders = orders_of(count)
    flips = jnp.array([flips_of(order) for order in orders], jnp.int32)
    ids = lax.rem((place ^ flips) + side * (count // 2), count)
    sent = weight_blocks(ids[:, : count // 2], mine, other, right, rows, edges)
    kept = weight_blocks(ids[:, count // 2 :], mine, other, right, rows, edges)
    parts = [exchange_sum(a, b, order) for a, b, order in zip(sent, kept, orders)]
    return jnp.concatenate(parts, axis=0)


def cube_sum(block, count):
    bit = 1
    while bit < count:
        block = block + lax.ppermute(block, "sp", [(i, i ^ bit) for i in range(count)])
        bit *= 2
    return block


def with_halo(block, width):
    count = lax.axis_size("sp")
    forward = [(i, i + 1) for i in range(count - 1)]
    backward = [(target, source) for source, target in forward]
    low = lax.ppermute(block[block.shape[0] - width :], "sp", forward)
    high = lax.ppermute(block[:width], "sp", backward)
    return jnp.concatenate([low, block, high], axis=0)


def swap(block):
    return lax.ppermute(block, "tp", [(0, 1), (1, 0)])


def on_device(features, weight_value, weight_gate, weight_out, conv_taps, norm_gain, out_grad):
    count = lax.axis_size("sp")
    place, side = lax.axis_index("sp"), lax.axis_index("tp")
    wide = features.shape[1]

    other_inputs = swap(features)
    other_cotangent = swap(out_grad)

    def project(mine, other, weight):
        own = lax.dynamic_slice_in_dim(weight, side * wide, wide, 0)
        far = lax.dynamic_slice_in_dim(weight, (1 - side) * wide, wide, 0)
        return jnp.dot(mine, own, preferred_element_type=jnp.float32) + jnp.dot(
            other, far, preferred_element_type=jnp.float32
        )

    value_half = project(features, other_inputs, weight_value).astype(jnp.bfloat16)
    gate_half = project(features, other_inputs, weight_gate).astype(jnp.bfloat16)
    value_half, gate_half = lax.optimization_barrier((value_half, gate_half))
    value_pre = value_half.astype(jnp.float32)
    gate_pre = gate_half.astype(jnp.float32)
    gate_sig = jax.nn.sigmoid(gate_pre)
    mixed_half = lax.optimization_barrier((value_pre * gate_sig).astype(jnp.bfloat16))
    tap_count = conv_taps.shape[0]
    half_width = tap_count // 2
    row_count = mixed_half.shape[0]
    channels = mixed_half.shape[1] * 2
    extended = with_halo(mixed_half, half_width).astype(jnp.float32)
    conv_out = jnp.zeros(mixed_half.shape, jnp.float32)
    for offset in range(tap_count):
        conv_out = conv_out + conv_taps[offset] * extended[offset : offset + row_count]
    sums = jnp.stack([jnp.sum(conv_out, axis=-1), jnp.sum(conv_out * conv_out, axis=-1)])
    row_sum, row_square = sums + swap(sums)
    mean_row = row_sum[:, None] / channels
    var_row = row_square[:, None] / channels - mean_row * mean_row
    inv_std = lax.rsqrt(var_row + NORM_EPS)
    normed = (conv_out - mean_row) * inv_std
    pre_act = normed * norm_gain
    act_sig = jax.nn.sigmoid(pre_act)
    act_half = lax.optimization_barrier((pre_act * act_sig).astype(jnp.bfloat16))
    act_grad = project(out_grad, other_cotangent, weight_out)
    pre_grad = act_grad * act_sig * (1.0 + pre_act * (1.0 - act_sig))
    gain_part = jnp.sum(pre_grad * normed, axis=0)
    norm_grad = pre_grad * norm_gain
    sums = jnp.stack([jnp.sum(norm_grad, axis=-1), jnp.sum(norm_grad * normed, axis=-1)])
    first_sum, second_sum = sums + swap(sums)
    first_mom = first_sum[:, None] / channels
    second_mom = second_sum[:, None] / channels
    conv_grad = inv_std * (norm_grad - first_mom - normed * second_mom)
    grad_ext = with_halo(conv_grad, half_width)
    mixed_grad = jnp.zeros(conv_grad.shape, jnp.float32)
    taps_rows = []
    for offset in range(tap_count):
        begin = 2 * half_width - offset
        mixed_grad = mixed_grad + conv_taps[offset] * grad_ext[begin : begin + row_count]
        taps_rows.append(jnp.sum(conv_grad * extended[offset : offset + row_count], axis=0))
    small = cube_sum(jnp.stack(taps_rows + [gain_part]), count)
    taps_grad, gain_grad = small[:tap_count], small[tap_count]
    value_grad = mixed_grad * gate_sig
    gate_grad = mixed_grad * value_pre * gate_sig * (1.0 - gate_sig)
    both_low = jnp.concatenate(
        [value_grad.astype(jnp.bfloat16), gate_grad.astype(jnp.bfloat16)], axis=1
    )
    both_low = lax.optimization_barrier(both_low)

    out_wgrad = scatter_rows(
        out_grad, other_cotangent, act_half.T, (4, 10), side, place, count
    )
    joined = scatter_rows(features, other_inputs, both_low.T, (4, 10), side, place, count)
    split_at = joined.shape[0] // 2
    return (
        value_grad,
        gate_grad,
        joined[:split_at].T,
        joined[split_at:].T,
        out_wgrad.T,
        taps_grad,
        gain_grad,
    )


def solution(mesh):
    in_specs = (
        P("sp", "tp"),
        P(None, "tp"),
        P(None, "tp"),
        P(None, "tp"),
        P(None, "tp"),
        P("tp"),
        P("sp", "tp"),
    )
    out_specs = (
        P("sp", "tp"),
        P("sp", "tp"),
        P("sp", "tp"),
        P("sp", "tp"),
        P("sp", "tp"),
        P(None, "tp"),
        P("tp"),
    )
    return jax.shard_map(
        on_device, mesh=mesh, in_specs=in_specs, out_specs=out_specs, check_vma=False
    )
```

```python
import functools

import jax
import jax.numpy as jnp
from jax import lax
from jax.experimental import pallas as pl
from jax.experimental.pallas import tpu as pltpu
from jax.sharding import PartitionSpec as P

NORM_EPS = 1e-05
LANES = 128
TILE = 32
PAD = 16

VMEM = pl.BlockSpec(memory_space=pltpu.VMEM)
SMEM = pl.BlockSpec(memory_space=pltpu.SMEM)


def shape_of(shape, dtype=jnp.float32):
    return jax.ShapeDtypeStruct(shape, dtype)


def lanes_of(chunk):
    return pl.ds(pl.multiple_of(chunk * LANES, LANES), LANES)


def rows_of(step, tile):
    return pl.ds(pl.multiple_of(step * tile, tile), tile)


def shifted_windows(window, offsets, tile):
    height = window.shape[0]
    for shift in range(8):
        group = [(k, j) for k, j in enumerate(offsets) if j % 8 == shift]
        if not group:
            continue
        moved = pltpu.roll(window, height - shift, 0) if shift else window
        for k, j in group:
            yield k, moved[j - shift : j - shift + tile]


def tap_sum(window, taps_ref, lanes, offsets, tile):
    total = jnp.zeros((tile, LANES), jnp.float32)
    for k, piece in shifted_windows(window, offsets, tile):
        total = total + taps_ref[k : k + 1, lanes] * piece
    return total


def pair_columns(first, second):
    shape = (first.shape[0], LANES)
    lane = lax.broadcasted_iota(jnp.int32, shape, 1)
    return jnp.where(lane == 0, jnp.broadcast_to(first, shape), jnp.broadcast_to(second, shape))


def joined_left(main_ref, halo_ref, spots):
    return jnp.concatenate([main_ref[...], *(halo_ref[a:b] for a, b in spots)], axis=0)


def forward_kernel(
    side_ref, mine_ref, mine_halo_ref, other_ref, other_halo_ref, value_w_ref, gate_w_ref, taps_ref,
    value_ref, gate_ref, mixed_ref, conv_ref, stats_ref, value_acc, gate_acc, *, spots, offsets,
):
    del side_ref
    step, steps = pl.program_id(0), pl.num_programs(0)

    def accumulate(main_ref, halo_ref, first):
        left = joined_left(main_ref, halo_ref, spots)
        for acc, weight_ref in ((value_acc, value_w_ref), (gate_acc, gate_w_ref)):
            term = jnp.dot(left, weight_ref[...], preferred_element_type=jnp.float32)
            acc[...] = term if first else acc[...] + term

    @pl.when(step == 0)
    def _():
        accumulate(mine_ref, mine_halo_ref, True)

    @pl.when((step > 0) & (step < steps // 2))
    def _():
        accumulate(mine_ref, mine_halo_ref, False)

    @pl.when(step >= steps // 2)
    def _():
        accumulate(other_ref, other_halo_ref, False)

    @pl.when(step == steps - 1)
    def _():
        main = value_ref.shape[0]
        halo = (mixed_ref.shape[0] - main) // 2

        def gated(source, target, store):
            value = value_acc[source].astype(jnp.bfloat16)
            gate = gate_acc[source].astype(jnp.bfloat16)
            if store is not None:
                value_ref[store] = value
                gate_ref[store] = gate
            sig = jax.nn.sigmoid(gate.astype(jnp.float32))
            mixed = (value.astype(jnp.float32) * sig).astype(jnp.bfloat16)
            mixed_ref[target] = mixed.astype(jnp.float32)

        gated(pl.ds(main, halo), pl.ds(0, halo), None)
        gated(pl.ds(main + halo, halo), pl.ds(main + halo, halo), None)

        @pl.loop(0, main // TILE)
        def _(tile):
            here = rows_of(tile, TILE)
            there = pl.ds(pl.multiple_of(halo + tile * TILE, TILE), TILE)
            gated(here, there, here)

        channels = value_ref.shape[1]

        @pl.loop(0, conv_ref.shape[0] // TILE)
        def _(tile):
            here = rows_of(tile, TILE)
            window_rows = pl.ds(pl.multiple_of(tile * TILE, TILE), TILE + 2 * PAD)
            total = jnp.zeros((TILE, LANES), jnp.float32)
            square = jnp.zeros((TILE, LANES), jnp.float32)
            for chunk in range(channels // LANES):
                lanes = pl.ds(chunk * LANES, LANES)
                out = tap_sum(mixed_ref[window_rows, lanes], taps_ref, lanes, offsets, TILE)
                conv_ref[here, lanes] = out
                total = total + out
                square = square + out * out
            stats_ref[here] = pair_columns(
                jnp.sum(total, axis=1, keepdims=True), jnp.sum(square, axis=1, keepdims=True)
            )


def forward(side, mine, mine_halo, other, other_halo, value_w, gate_w, taps, spots, offsets):
    tokens, wide = mine.shape
    channels = value_w.shape[1]
    halo_rows = mine_halo.shape[0]
    extra = sum(b - a for a, b in spots)
    depth = wide // 2
    half = wide // depth
    mine_map = lambda k, s: (0, jnp.minimum(k, half - 1))
    other_map = lambda k, s: (0, jnp.maximum(k - half, 0))
    weight_map = lambda k, s: (lax.rem(k + half * s[0], 2 * half), 0)
    whole = lambda k, s: (0, 0)
    outs = (
        shape_of((tokens, channels), jnp.bfloat16),
        shape_of((tokens, channels), jnp.bfloat16),
        shape_of((tokens + extra, channels)),
        shape_of((tokens + 2 * PAD, channels)),
        shape_of((tokens + 2 * PAD, LANES)),
    )
    return pl.pallas_call(
        functools.partial(forward_kernel, spots=spots, offsets=offsets),
        grid_spec=pltpu.PrefetchScalarGridSpec(
            num_scalar_prefetch=1,
            grid=(2 * half,),
            in_specs=[
                pl.BlockSpec((tokens, depth), mine_map),
                pl.BlockSpec((halo_rows, depth), mine_map),
                pl.BlockSpec((tokens, depth), other_map),
                pl.BlockSpec((halo_rows, depth), other_map),
                pl.BlockSpec((depth, channels), weight_map),
                pl.BlockSpec((depth, channels), weight_map),
                pl.BlockSpec(taps.shape, whole),
            ],
            out_specs=[pl.BlockSpec(o.shape, whole) for o in outs],
            scratch_shapes=[pltpu.VMEM((tokens + extra, channels), jnp.float32)] * 2,
        ),
        out_shape=outs,
        cost_estimate=pl.CostEstimate(
            flops=8 * (tokens + extra) * wide * channels, bytes_accessed=16 * 2**20, transcendentals=0
        ),
        name="forward",
    )(side, mine, mine_halo, other, other_halo, value_w, gate_w, taps)


def product_kernel(
    side_ref, mine_ref, mine_halo_ref, other_ref, other_halo_ref, weight_ref, out_ref, acc, *, spots
):
    del side_ref
    step, steps = pl.program_id(0), pl.num_programs(0)

    def accumulate(main_ref, halo_ref, first):
        left = joined_left(main_ref, halo_ref, spots)
        term = jnp.dot(left, weight_ref[...], preferred_element_type=jnp.float32)
        acc[...] = term if first else acc[...] + term

    @pl.when(step == 0)
    def _():
        accumulate(mine_ref, mine_halo_ref, True)

    @pl.when((step > 0) & (step < steps // 2))
    def _():
        accumulate(mine_ref, mine_halo_ref, False)

    @pl.when(step >= steps // 2)
    def _():
        accumulate(other_ref, other_halo_ref, False)

    @pl.when(step == steps - 1)
    def _():
        main = mine_ref.shape[0]
        halo = (out_ref.shape[0] - main) // 2
        out_ref[0:halo] = acc[main : main + halo]
        out_ref[halo : halo + main] = acc[0:main]
        out_ref[halo + main : main + 2 * halo] = acc[main + halo : main + 2 * halo]


def product(side, mine, mine_halo, other, other_halo, weight, spots):
    tokens, wide = mine.shape
    channels = weight.shape[1]
    halo_rows = mine_halo.shape[0]
    extra = sum(b - a for a, b in spots)
    depth = wide // 2
    half = wide // depth
    mine_map = lambda k, s: (0, jnp.minimum(k, half - 1))
    other_map = lambda k, s: (0, jnp.maximum(k - half, 0))
    return pl.pallas_call(
        functools.partial(product_kernel, spots=spots),
        grid_spec=pltpu.PrefetchScalarGridSpec(
            num_scalar_prefetch=1,
            grid=(2 * half,),
            in_specs=[
                pl.BlockSpec((tokens, depth), mine_map),
                pl.BlockSpec((halo_rows, depth), mine_map),
                pl.BlockSpec((tokens, depth), other_map),
                pl.BlockSpec((halo_rows, depth), other_map),
                pl.BlockSpec((depth, channels), lambda k, s: (lax.rem(k + half * s[0], 2 * half), 0)),
            ],
            out_specs=pl.BlockSpec((tokens + extra, channels), lambda k, s: (0, 0)),
            scratch_shapes=[pltpu.VMEM((tokens + extra, channels), jnp.float32)],
        ),
        out_shape=shape_of((tokens + extra, channels)),
        cost_estimate=pl.CostEstimate(
            flops=4 * (tokens + extra) * wide * channels, bytes_accessed=9 * 2**20, transcendentals=0
        ),
        name="product",
    )(side, mine, mine_halo, other, other_halo, weight)


def norm_of(stats, channels):
    mean = stats[:, 0:1] / channels
    var = stats[:, 1:2] / channels - mean * mean
    return mean, lax.rsqrt(var + NORM_EPS)


def middle_kernel(
    conv_ref, stats_ref, far_stats_ref, act_grad_ref, gain_ref,
    act_ref, norm_grad_ref, sums_ref, gain_part_ref, act_all, gain_acc, *, channels,
):
    tiles = conv_ref.shape[0] // PAD
    gain_acc[...] = jnp.zeros_like(gain_acc)

    @pl.loop(0, tiles)
    def _(tile):
        here = rows_of(tile, PAD)
        mean, inv_std = norm_of(stats_ref[here] + far_stats_ref[here], channels)
        gain = gain_ref[...]
        normed = (conv_ref[here] - mean) * inv_std
        pre_act = normed * gain
        sig = jax.nn.sigmoid(pre_act)
        act_all[here] = pre_act * sig
        pre_grad = act_grad_ref[here] * sig * (1.0 + pre_act * (1.0 - sig))
        inside = (tile > 0) & (tile < tiles - 1)
        gain_acc[...] += jnp.where(inside, pre_grad * normed, 0.0)
        norm_grad = pre_grad * gain
        norm_grad_ref[here] = norm_grad
        sums_ref[here] = pair_columns(
            jnp.sum(norm_grad, axis=1, keepdims=True),
            jnp.sum(norm_grad * normed, axis=1, keepdims=True),
        )

    gain_part_ref[...] = jnp.sum(gain_acc[...], axis=0, keepdims=True)
    width, tokens = act_ref.shape

    @pl.loop(0, tokens // LANES)
    def _(block):
        source = pl.ds(pl.multiple_of(PAD + block * LANES, PAD), LANES)
        for chunk in range(width // LANES):
            lanes = pl.ds(chunk * LANES, LANES)
            act_ref[lanes, lanes_of(block)] = act_all[source, lanes].T.astype(jnp.bfloat16)


def middle(conv, stats, far_stats, act_grad, gain, channels):
    rows, width = conv.shape
    tokens = rows - 2 * PAD
    return pl.pallas_call(
        functools.partial(middle_kernel, channels=channels),
        in_specs=[VMEM] * 5,
        out_specs=[VMEM] * 4,
        out_shape=(
            shape_of((width, tokens), jnp.bfloat16),
            shape_of((rows, width)),
            shape_of((rows, LANES)),
            shape_of((1, width)),
        ),
        scratch_shapes=[
            pltpu.VMEM((rows, width), jnp.float32),
            pltpu.VMEM((PAD, width), jnp.float32),
        ],
        cost_estimate=pl.CostEstimate(
            flops=4 * 10**9, bytes_accessed=16 * rows * width, transcendentals=2 * rows * width
        ),
        name="middle",
    )(conv, stats, far_stats, act_grad, gain)


def conv_grad_kernel(
    inside_ref, conv_ref, stats_ref, far_stats_ref, norm_grad_ref, sums_ref, far_sums_ref, mixed_ref,
    gain_part_ref, conv_grad_ref, small_ref, *, channels, offsets,
):
    rows, width = conv_ref.shape
    tiles = rows // PAD

    @pl.loop(0, tiles)
    def _(tile):
        here = rows_of(tile, PAD)
        mean, inv_std = norm_of(stats_ref[here] + far_stats_ref[here], channels)
        normed = (conv_ref[here] - mean) * inv_std
        sums = sums_ref[here] + far_sums_ref[here]
        first, second = sums[:, 0:1] / channels, sums[:, 1:2] / channels
        grad = inv_std * (norm_grad_ref[here] - first - normed * second)
        outside = ((tile == 0) & (inside_ref[0] == 0)) | (
            (tile == tiles - 1) & (inside_ref[1] == 0)
        )
        conv_grad_ref[here] = jnp.where(outside, 0.0, grad)

    taps = len(offsets)
    shift = (mixed_ref.shape[0] - rows) // 2

    @pl.loop(0, width // LANES)
    def _(chunk):
        lanes = lanes_of(chunk)

        def body(tile, sums):
            start = pl.multiple_of(tile * TILE, TILE)
            grad = conv_grad_ref[pl.ds(pl.multiple_of(start + PAD, PAD), TILE), lanes]
            window = mixed_ref[pl.ds(pl.multiple_of(start + shift, 8), TILE + 2 * PAD), lanes]
            sums = list(sums)
            for k, piece in shifted_windows(window, offsets, TILE):
                term = grad * piece
                total = sums[k]
                for row in range(0, TILE, 8):
                    total = total + term[row : row + 8]
                sums[k] = total
            return tuple(sums)

        zero = jnp.zeros((8, LANES), jnp.float32)
        sums = lax.fori_loop(0, (rows - 2 * PAD) // TILE, body, (zero,) * taps)
        for k, total in enumerate(sums):
            small_ref[k : k + 1, lanes] = jnp.sum(total, axis=0, keepdims=True)
        small_ref[taps : taps + 1, lanes] = gain_part_ref[:, lanes]


def conv_gradient(inside, conv, stats, far_stats, norm_grad, sums, far_sums, mixed, gain_part, channels, offsets):
    rows, width = conv.shape
    return pl.pallas_call(
        functools.partial(conv_grad_kernel, channels=channels, offsets=offsets),
        in_specs=[SMEM] + [VMEM] * 8,
        out_specs=[VMEM] * 2,
        out_shape=(shape_of((rows, width)), shape_of((len(offsets) + 1, width))),
        cost_estimate=pl.CostEstimate(
            flops=6 * 10**9, bytes_accessed=16 * rows * width, transcendentals=0
        ),
        name="conv_grad",
    )(inside, conv, stats, far_stats, norm_grad, sums, far_sums, mixed, gain_part)


def backward_kernel(
    conv_grad_ref, taps_ref, value_ref, gate_ref, value_grad_ref, gate_grad_ref, low_ref, *, offsets
):
    tokens, width = value_ref.shape

    @pl.loop(0, width // LANES)
    def _(chunk):
        lanes = lanes_of(chunk)

        @pl.loop(0, tokens // LANES)
        def _(block):
            for part in range(LANES // TILE):
                start = pl.multiple_of(block * LANES + part * TILE, TILE)
                here = pl.ds(start, TILE)
                window = conv_grad_ref[pl.ds(start, TILE + 2 * PAD), lanes]
                mixed_grad = tap_sum(window, taps_ref, lanes, offsets, TILE)
                value = value_ref[here, lanes].astype(jnp.float32)
                sig = jax.nn.sigmoid(gate_ref[here, lanes].astype(jnp.float32))
                value_grad_ref[here, lanes] = mixed_grad * sig
                gate_grad_ref[here, lanes] = mixed_grad * value * sig * (1.0 - sig)
            there = lanes_of(block)
            below = pl.ds(pl.multiple_of(width + chunk * LANES, LANES), LANES)
            low_ref[lanes, there] = value_grad_ref[there, lanes].T.astype(jnp.bfloat16)
            low_ref[below, there] = gate_grad_ref[there, lanes].T.astype(jnp.bfloat16)


def backward(conv_grad, taps, value, gate, offsets):
    tokens, width = value.shape
    return pl.pallas_call(
        functools.partial(backward_kernel, offsets=offsets),
        in_specs=[VMEM] * 4,
        out_specs=[VMEM] * 3,
        out_shape=(
            shape_of((tokens, width)),
            shape_of((tokens, width)),
            shape_of((2 * width, tokens), jnp.bfloat16),
        ),
        cost_estimate=pl.CostEstimate(
            flops=6 * 10**9, bytes_accessed=18 * tokens * width, transcendentals=0
        ),
        name="backward",
    )(conv_grad, taps, value, gate)


def weight_kernel(ids_ref, mine_ref, other_ref, right_ref, *outs, edges):
    rows = outs[0].shape[2]
    blocks = outs[0].shape[0]
    half = mine_ref.shape[1] // rows

    def fill(left_ref, spot, out_ref, step, begin, end):
        columns = pl.ds(pl.multiple_of(spot * rows, rows), rows)
        term = jnp.dot(
            right_ref[begin:end], left_ref[:, columns], preferred_element_type=jnp.float32
        )
        out_ref[step] = term.astype(jnp.bfloat16)

    @pl.loop(0, blocks)
    def _(step):
        for k, out_ref in enumerate(outs):
            spot = ids_ref[k, step]
            near = spot < half
            begin, end = edges[k], edges[k + 1]

            @pl.when(near)
            def _():
                fill(mine_ref, spot, out_ref, step, begin, end)

            @pl.when(jnp.logical_not(near))
            def _():
                fill(other_ref, spot - half, out_ref, step, begin, end)


def weight_blocks(ids, mine, other, right, rows, edges):
    tokens = right.shape[1]
    blocks = ids.shape[1]
    if rows % 128:
        whole = jnp.concatenate([mine, other], axis=1).reshape(tokens, -1, rows)
        return [
            jnp.einsum(
                "ct,tbr->bcr", right[a:b], whole[:, spots], preferred_element_type=jnp.float32
            ).astype(jnp.bfloat16)
            for a, b, spots in zip(edges[:-1], edges[1:], ids)
        ]
    whole = pl.BlockSpec(memory_space=pltpu.VMEM)
    return pl.pallas_call(
        functools.partial(weight_kernel, edges=edges),
        in_specs=[pl.BlockSpec(memory_space=pltpu.SMEM), whole, whole, whole],
        out_specs=[whole] * ids.shape[0],
        out_shape=[
            jax.ShapeDtypeStruct((blocks, b - a, rows), jnp.bfloat16)
            for a, b in zip(edges[:-1], edges[1:])
        ],
        cost_estimate=pl.CostEstimate(
            flops=2 * tokens * rows * edges[-1] * blocks,
            bytes_accessed=4 * mine.size + 2 * right.size + 2 * blocks * edges[-1] * rows,
            transcendentals=0,
        ),
    )(ids, mine, other, right)


def add(terms):
    total = terms[0].astype(jnp.float32)
    for term in terms[1:]:
        total = total + term.astype(jnp.float32)
    return total


def flips_of(order):
    bits = len(order)
    return [
        sum(1 << bit for k, bit in enumerate(order) if not (p >> (bits - 1 - k)) & 1)
        for p in range(1 << bits)
    ]


def exchange_sum(sent, kept, order):
    count = 1 << len(order)
    kept = [kept]
    for step, bit in enumerate(order):
        got = lax.ppermute(sent, "sp", [(i, i ^ (1 << bit)) for i in range(count)])
        kept.append(got)
        size = got.shape[0]
        if step + 1 < len(order):
            sent = add([k[: size // 2] for k in kept]).astype(jnp.bfloat16)
            kept = [k[size // 2 :] for k in kept]
    return add([k[0] for k in kept])


def orders_of(count):
    bits = count.bit_length() - 1
    top = list(range(max(bits - 2, 0), bits))
    low = list(range(max(bits - 2, 0)))
    return top + low, low + top, low[::-1] + top


def scatter_rows(mine, other, right, splits, side, place, count):
    rows = 2 * mine.shape[1] // count
    columns = right.shape[0]
    edges = (0, *(columns * s // 16 for s in splits), columns)
    orders = orders_of(count)
    flips = jnp.array([flips_of(order) for order in orders], jnp.int32)
    ids = lax.rem((place ^ flips) + side * (count // 2), count)
    sent = weight_blocks(ids[:, : count // 2], mine, other, right, rows, edges)
    kept = weight_blocks(ids[:, count // 2 :], mine, other, right, rows, edges)
    parts = [exchange_sum(a, b, order) for a, b, order in zip(sent, kept, orders)]
    return jnp.concatenate(parts, axis=0)


def cube_steps(block, count, bits):
    for bit in bits:
        block = block + lax.ppermute(block, "sp", [(i, i ^ (1 << bit)) for i in range(count)])
    return block


def swap(block):
    return lax.ppermute(block, "tp", [(0, 1), (1, 0)])


def on_device(features, weight_value, weight_gate, weight_out, conv_taps, norm_gain, out_grad):
    count = lax.axis_size("sp")
    place, side = lax.axis_index("sp"), lax.axis_index("tp")
    tap_count = conv_taps.shape[0]
    half_width = tap_count // 2
    channels = 2 * weight_value.shape[1]
    forward_offsets = tuple(k - half_width + PAD for k in range(tap_count))
    backward_offsets = tuple(half_width - k + PAD for k in range(tap_count))

    up = [(i, i + 1) for i in range(count - 1)]
    down = [(b, a) for a, b in up]
    low = lax.ppermute(jnp.concatenate([features[-2 * PAD :], out_grad[-PAD:]], axis=0), "sp", up)
    high = lax.ppermute(jnp.concatenate([features[: 2 * PAD], out_grad[:PAD]], axis=0), "sp", down)
    halo = jnp.concatenate([low, high], axis=0)
    other_inputs = swap(features)
    other_halo = swap(halo)
    other_cotangent = swap(out_grad)
    side_of = side.reshape(1).astype(jnp.int32)
    inside = jnp.stack([place > 0, place < count - 1]).astype(jnp.int32)

    value_half, gate_half, mixed, conv_out, stats = forward(
        side_of, features, halo, other_inputs, other_halo, weight_value, weight_gate, conv_taps,
        ((0, 2 * PAD), (3 * PAD, 5 * PAD)), forward_offsets,
    )
    far_stats = swap(stats)
    act_grad = product(
        side_of, out_grad, halo, other_cotangent, other_halo, weight_out,
        ((2 * PAD, 3 * PAD), (5 * PAD, 6 * PAD)),
    )
    act_half, norm_grad, sums, gain_part = middle(
        conv_out, stats, far_stats, act_grad, norm_gain[None], channels
    )
    far_sums = swap(sums)
    out_wgrad = scatter_rows(out_grad, other_cotangent, act_half, (4, 10), side, place, count)
    conv_grad, small = conv_gradient(
        inside, conv_out, stats, far_stats, norm_grad, sums, far_sums, mixed, gain_part, channels,
        forward_offsets,
    )
    small = cube_steps(small, count, range(count.bit_length() - 1))
    taps_grad, gain_grad = small[:tap_count], small[tap_count]
    value_grad, gate_grad, low_half = backward(
        conv_grad, conv_taps, value_half, gate_half, backward_offsets
    )
    joined = scatter_rows(features, other_inputs, low_half, (4, 10), side, place, count)
    split_at = joined.shape[0] // 2
    return (
        value_grad,
        gate_grad,
        joined[:split_at].T,
        joined[split_at:].T,
        out_wgrad.T,
        taps_grad,
        gain_grad,
    )


def solution(mesh):
    in_specs = (
        P("sp", "tp"),
        P(None, "tp"),
        P(None, "tp"),
        P(None, "tp"),
        P(None, "tp"),
        P("tp"),
        P("sp", "tp"),
    )
    out_specs = (
        P("sp", "tp"),
        P("sp", "tp"),
        P("sp", "tp"),
        P("sp", "tp"),
        P("sp", "tp"),
        P(None, "tp"),
        P("tp"),
    )
    return jax.shard_map(
        on_device, mesh=mesh, in_specs=in_specs, out_specs=out_specs, check_vma=False
    )
```
